256 devices in a mesh: ep: 128 (over z, y, x), tp: 2 (over core).
Axes of the slice: x: 4, y: 4, z: 8, core: 2. Of those that a mesh axis runs over, the one named last changes fastest.
Arguments:
- tokens: bfloat16 [2048, 1024], P('ep'), may hold values from -6 to 6
- mixer_gain: float32 [1024], replicated, may hold values from 0.1 to 1.9
- query_weight: bfloat16 [1024, 1024], P(None, 'tp'), may hold values from -0.1875 to 0.1875
- key_weight: bfloat16 [1024, 256], P(None, 'tp'), may hold values from -0.1875 to 0.1875
- value_weight: bfloat16 [1024, 256], P(None, 'tp'), may hold values from -0.1875 to 0.1875
- head_lambda: float32 [8], P('tp'), may hold values from 0.3 to 0.8
- head_gain: float32 [128], replicated, may hold values from 0.1 to 1.9
- out_weight: bfloat16 [1024, 1024], P('tp'), may hold values from -0.1875 to 0.1875
- cache_keys: bfloat16 [2048, 1024, 256], P('ep', None, 'tp'), may hold values from -700 to 700
- cache_values: bfloat16 [2048, 1024, 256], P('ep', None, 'tp'), may hold values from -6 to 6
- seq_lengths: int32 [2048], P('ep'), may hold values from 2 to 1024, as said below
- channel_gain: float32 [1024], replicated, may hold values from 0.1 to 1.9
- expert_ids: int32 [2048, 6], P('ep'), may hold values from 0 to 127, all different within a row; in each aligned block of 16 rows (0 to 15, 16 to 31, ...) at most 2 rows name the same one
- expert_shares: bfloat16 [2048, 6], P('ep'), may hold values from 0.19921875 to 1
- expert_gate: bfloat16 [128, 1024, 256], P('ep', None, 'tp'), may hold values from -0.1875 to 0.1875
- expert_up: bfloat16 [128, 1024, 256], P('ep', None, 'tp'), may hold values from -0.1875 to 0.1875
- expert_down: bfloat16 [128, 256, 1024], P('ep', 'tp'), may hold values from -0.375 to 0.375
- dense_gate: bfloat16 [1024, 4096], P('tp', 'ep'), may hold values from -0.1875 to 0.1875
- dense_up: bfloat16 [1024, 4096], P('tp', 'ep'), may hold values from -0.1875 to 0.1875
- dense_down: bfloat16 [4096, 1024], P('ep', 'tp'), may hold values from -0.1875 to 0.1875
- branch_gate: float32 [1024], replicated, may hold values from -0.1875 to 0.1875
Outputs:
- layer_out: bfloat16 [2048, 1024], P('ep', 'tp')
The draws below stay inside these ranges and needn't reach their ends.
Inputs may be any that keep to these rules, and one draw needn't show every extreme that they name: `expert_ids`: each row names 6 different experts; among the 16 rows of one index of ep no expert is named by more than 2 rows. `seq_lengths`: some sequence has all 1024 positions live.
All inputs are finite; a program needn't handle non-finite values.
Results may differ from the reference program's by a relative error of at most 0.017.
The reference program's roundings to bfloat16 on the way count: a program that leaves them out, or rounds other values in their place, can miss the bound.
Values may be sent and summed in bfloat16 or wider, within the bound.
No kernel may reach another device: no remote copies, remote signals or barrier semaphores. Data moves between devices by JAX's collectives and lax.ppermute only.
A program may use at most 64 MiB of HBM per device.

```python
import math
import jax
import jax.numpy as jnp
import numpy as np
from jax import lax

D = 1024
H = 8
KG = 2
HD = 64
VD = 128
F = 256
DH = 4096
TOP_K = 6
SEQ_DEV = 16
CACHE_LEN = 1024
BATCH = 2048
EXPERTS = 128
CAP = 2
N_EP = 128


def draw_cache_keys(key, part):
    base_key = jax.random.fold_in(key, 17)
    first_key = jax.random.fold_in(base_key, 0)
    normal_draw = jnp.clip(jax.random.normal(first_key, (BATCH, CACHE_LEN, KG * 2 * HD), jnp.float32), -6.0, 6.0) * 1.75
    return normal_draw.astype(jnp.bfloat16)


def draw_seq_lengths(key, part):
    base_key = jax.random.fold_in(key, 29)
    first_key, second_key = jax.random.split(base_key)
    base_draw = jax.random.randint(first_key, (BATCH,), 0, CACHE_LEN - 1)
    level_draw = jax.random.randint(second_key, (BATCH // SEQ_DEV,), 1, 5)
    levels = jnp.repeat(level_draw, SEQ_DEV)
    lengths = 2 + base_draw * levels // 4
    lengths = lengths.at[0].set(CACHE_LEN)
    return lengths.astype(jnp.int32)


def shard_levels(rng, dims, shards, smallest, top_value):
    loudness, own = 1.0, jax.random.fold_in(rng, 6)
    for dim, blocks in shards:
        draws = jnp.exp(jax.random.uniform(jax.random.fold_in(own, dim), (blocks,), jnp.float32, smallest / len(shards), top_value / len(shards)))
        loudness = loudness * jnp.repeat(draws, dims[dim] // blocks).reshape([-1 if axis == dim else 1 for axis in range(len(dims))])
    return loudness


def routed_block(stream_key, own, number, rows, count, top, most, slope):
    order = jax.random.permutation(stream_key, count)
    heavy_load, ordinary = portions_of(count, rows * top, most, slope, True), portions_of(count, rows * top, most, slope, False)
    places = jnp.arange(count)

    def named(sizes, offset_by):
        used = int((sizes > 0).sum())
        fixed = max(1, used // 4)
        moved = fixed + (places - fixed + offset_by * (used - fixed)) % max(1, count - fixed)
        return jnp.zeros((count,), jnp.int32).at[order[jnp.where(places < fixed, places, moved)]].set(jnp.asarray(sizes, jnp.int32))

    sizes = jnp.where(number % 4 == 0, named(heavy_load, number // 4), named(ordinary, number - number // 4 - 1))
    mixed = jax.random.permutation(jax.random.fold_in(own, 3), count)
    donor, receiver = mixed[0:count // 2 * 2:2], mixed[1:count // 2 * 2:2]
    room = jnp.minimum(sizes[donor] - 1, most - sizes[receiver]) // 2
    room = jnp.where((donor == order[0]) | (receiver == order[0]) | (sizes[receiver] == 0), 0, jnp.maximum(room, 0))
    moved = jax.random.randint(jax.random.fold_in(own, 4), (count // 2,), 0, 1 << 20) % (room + 1)
    sizes = sizes.at[donor].add(-moved).at[receiver].add(moved)
    members = jnp.searchsorted(jnp.cumsum(sizes), jnp.arange(rows * top), side="right").astype(jnp.int32)
    table = members.reshape(top, rows).T
    table = table[jax.random.permutation(jax.random.fold_in(own, 1), rows)]
    offset_by = jax.random.randint(jax.random.fold_in(own, 2), (rows, 1), 0, top)
    return jnp.take_along_axis(table, (jnp.arange(top)[None, :] + offset_by) % top, axis=1)


def portions_of(amount, total, limit, slope, full):
    weights = [(1 << 20) // math.isqrt(standing ** slope) + 1 for standing in range(1, amount + 1)]
    largest = limit if full else min(limit, max(-(-total // amount), total * weights[0] // sum(weights)))
    least = 1 if total - largest >= amount - 1 else 0
    given, rest = [largest] + [least] * (amount - 1), total - largest - least * (amount - 1)
    while rest > 0:
        candidates = [i for i in range(1, amount) if given[i] < largest] or [i for i in range(1, amount) if given[i] < limit]
        mass, remaining = sum([weights[i] for i in candidates]), rest
        for i in candidates:
            addition = min(limit - given[i], max(1, remaining * weights[i] // mass), rest)
            given[i] = given[i] + addition
            rest = rest - addition
    return np.array(given)


def normal_values(stream_key, dims, spread, reach, shards=(), kind=jnp.bfloat16):
    values = spread * jax.random.normal(stream_key, dims, jnp.float32)
    if shards:
        values = values * shard_levels(stream_key, dims, shards, -0.22, 0.18)
    return jnp.clip(values, -reach, reach).astype(kind)


def setup_inputs(seed: int = 0) -> dict:
    streams_of = jax.random.split(jax.random.key(seed), 22)
    tokens = normal_values(streams_of[0], (BATCH, D), 1.0, 6.0, ((0, 128),))
    mixer_gain = jnp.clip(1.0 + 0.18 * jax.random.normal(streams_of[1], (D,), jnp.float32), 0.1, 1.9)
    query_weight = normal_values(streams_of[2], (D, H * 2 * HD), D ** -0.5, 0.1875, ((1, 2),))
    key_weight = normal_values(streams_of[3], (D, KG * 2 * HD), D ** -0.5, 0.1875, ((1, 2),))
    value_weight = normal_values(streams_of[4], (D, KG * VD), D ** -0.5, 0.1875, ((1, 2),))
    head_lambda = jnp.clip(0.3 + 0.5 * jax.random.uniform(streams_of[5], (H,), jnp.float32) ** shard_levels(streams_of[5], (H,), ((0, 2),), -0.2, 0.2), 0.3, 0.8)
    head_gain = jnp.clip(1.0 + 0.18 * jax.random.normal(streams_of[6], (VD,), jnp.float32), 0.1, 1.9)
    out_weight = normal_values(streams_of[7], (H * VD, D), (H * VD) ** -0.5, 0.1875, ((0, 2),))
    cache_keys = draw_cache_keys(jax.random.fold_in(streams_of[21], 71), 0)
    cache_values = normal_values(streams_of[9], (BATCH, CACHE_LEN, KG * VD), 1.0, 6.0, ((0, 128), (2, 2)))
    seq_lengths = draw_seq_lengths(jax.random.fold_in(streams_of[21], 71), 0)
    channel_gain = jnp.clip(1.0 + 0.18 * jax.random.normal(streams_of[11], (D,), jnp.float32), 0.1, 1.9)
    expert_ids_keys = jax.random.split(jax.random.fold_in(streams_of[12], 1), BATCH // SEQ_DEV)
    expert_ids_turns = jax.random.permutation(jax.random.fold_in(streams_of[12], 3), BATCH // SEQ_DEV)
    expert_ids = jax.vmap(lambda own, number: routed_block(jax.random.fold_in(streams_of[12], 2), own, number, SEQ_DEV, EXPERTS, TOP_K, CAP, 2))(expert_ids_keys, expert_ids_turns).reshape((BATCH, TOP_K))
    expert_shares = jnp.clip(0.19921875 + 0.80078125 * jax.random.uniform(streams_of[13], (BATCH, TOP_K), jnp.float32) ** shard_levels(streams_of[13], (BATCH, TOP_K), ((0, 128),), -0.2, 0.2), 0.19921875, 1.0).astype(jnp.bfloat16)
    expert_gate = normal_values(streams_of[14], (EXPERTS, D, F), D ** -0.5, 0.1875, ((0, 128), (2, 2)))
    expert_up = normal_values(streams_of[15], (EXPERTS, D, F), D ** -0.5, 0.1875, ((0, 128), (2, 2)))
    expert_down = normal_values(streams_of[16], (EXPERTS, F, D), F ** -0.5, 0.375, ((0, 128), (1, 2)))
    dense_gate = normal_values(streams_of[17], (D, DH), D ** -0.5, 0.1875, ((0, 2), (1, 128)))
    dense_up = normal_values(streams_of[18], (D, DH), D ** -0.5, 0.1875, ((0, 2), (1, 128)))
    dense_down = normal_values(streams_of[19], (DH, D), (DH // 4) ** -0.5, 0.1875, ((0, 128), (1, 2)))
    branch_gate = normal_values(streams_of[20], (D,), D ** -0.5, 0.1875, (), jnp.float32)
    return dict(tokens=tokens, mixer_gain=mixer_gain, query_weight=query_weight, key_weight=key_weight, value_weight=value_weight, head_lambda=head_lambda, head_gain=head_gain, out_weight=out_weight, cache_keys=cache_keys, cache_values=cache_values, seq_lengths=seq_lengths, channel_gain=channel_gain, expert_ids=expert_ids, expert_shares=expert_shares, expert_gate=expert_gate, expert_up=expert_up, expert_down=expert_down, dense_gate=dense_gate, dense_up=dense_up, dense_down=dense_down, branch_gate=branch_gate)


NORM_EPS = 1e-06
HEAD_EPS = 1e-05
THETA = 500000.0
LAMBDA_BASE = 0.2

def norm_rows(values, gain_vec, epsilon):
    mean_square = lax.optimization_barrier(jnp.mean(values * values, axis=-1, keepdims=True))
    return values * lax.rsqrt(mean_square + epsilon) * gain_vec

def rotate(values, position):
    half_dim = HD // 2
    frequency = THETA ** (-jnp.arange(half_dim, dtype=jnp.float32) * (2.0 / HD))
    angles = position.astype(jnp.float32)[:, None] * frequency[None, :]
    cos_vals = jnp.cos(angles)[:, None, :]
    sin_vals = jnp.sin(angles)[:, None, :]
    first_half = values[..., :half_dim]
    second = values[..., half_dim:]
    return jnp.concatenate([first_half * cos_vals - second * sin_vals, second * cos_vals + first_half * sin_vals], axis=-1)

def widen(values):
    return values.astype(jnp.float32)

def reference(tokens, mixer_gain, query_weight, key_weight, value_weight, head_lambda, head_gain, out_weight, cache_keys, cache_values, seq_lengths, channel_gain, expert_ids, expert_shares, expert_gate, expert_up, expert_down, dense_gate, dense_up, dense_down, branch_gate):
    resid = widen(tokens)
    normed = norm_rows(resid, mixer_gain, NORM_EPS).astype(jnp.bfloat16)
    query_raw = jnp.dot(normed, query_weight, preferred_element_type=jnp.float32).reshape(BATCH, H * 2, HD)
    key_raw = jnp.dot(normed, key_weight, preferred_element_type=jnp.float32).reshape(BATCH, KG * 2, HD)
    value_new = jnp.dot(normed, value_weight, preferred_element_type=jnp.float32).astype(jnp.bfloat16)
    value_new = value_new.reshape(N_EP, SEQ_DEV, KG, VD)
    query = rotate(query_raw, seq_lengths).astype(jnp.bfloat16).reshape(N_EP, SEQ_DEV, KG, H // KG, 2, HD)
    key_new = rotate(key_raw, seq_lengths).astype(jnp.bfloat16).reshape(N_EP, SEQ_DEV, KG, 2, HD)
    lambdas = head_lambda.reshape(KG, H // KG)
    key_rows = cache_keys.reshape(N_EP, SEQ_DEV, CACHE_LEN, KG, 2, HD)
    value_rows = cache_values.reshape(N_EP, SEQ_DEV, CACHE_LEN, KG, VD)
    length_rows = seq_lengths.reshape(N_EP, SEQ_DEV)
    score_scale = HD ** (-0.5)

    def attend_block(pieces_in):
        query_blk, key_blk, value_blk, cache_key_blk, cache_value_blk, length_blk = pieces_in
        scores = jnp.einsum('sgjcd,slgcd->sgjcl', widen(query_blk), widen(cache_key_blk)) * score_scale
        fresh_score = jnp.einsum('sgjcd,sgcd->sgjc', widen(query_blk), widen(key_blk)) * score_scale
        live = jnp.arange(CACHE_LEN)[None, :] < length_blk[:, None]
        scores = jnp.where(live[:, None, None, None, :], scores, -jnp.inf)
        peak = jnp.maximum(lax.optimization_barrier(jnp.max(scores, axis=-1)), fresh_score)
        expo_scores = jnp.exp(scores - peak[..., None])
        expo_fresh = jnp.exp(fresh_score - peak)
        denom_sum = lax.optimization_barrier(jnp.sum(expo_scores, axis=-1)) + expo_fresh
        probability = expo_scores / denom_sum[..., None]
        prob_fresh = expo_fresh / denom_sum
        weight = (probability[:, :, :, 0] - lambdas[None, :, :, None] * probability[:, :, :, 1]).astype(jnp.bfloat16)
        weight_fresh = (prob_fresh[..., 0] - lambdas[None] * prob_fresh[..., 1]).astype(jnp.bfloat16)
        mixed_heads = jnp.einsum('sgjl,slgv->sgjv', widen(weight), widen(cache_value_blk))
        return mixed_heads + widen(weight_fresh)[..., None] * widen(value_blk)[:, :, None, :]
    head_mix = lax.map(attend_block, (query, key_new, value_new, key_rows, value_rows, length_rows))
    head_mix = head_mix.reshape(BATCH, H, VD)
    head_out = (norm_rows(head_mix, head_gain, HEAD_EPS) * (1.0 - LAMBDA_BASE)).astype(jnp.bfloat16)
    attn_sum = jnp.dot(head_out.reshape(BATCH, H * VD), out_weight, preferred_element_type=jnp.float32)
    resid_mid = (resid + attn_sum).astype(jnp.bfloat16)
    mid_wide = widen(resid_mid)
    ffn_input = norm_rows(mid_wide, channel_gain, NORM_EPS).astype(jnp.bfloat16)
    gate_value = jax.nn.sigmoid(jnp.dot(widen(ffn_input), branch_gate, precision=lax.Precision.HIGHEST))
    dense_gate_part = jnp.dot(ffn_input, dense_gate, preferred_element_type=jnp.float32)
    dense_up_part = jnp.dot(ffn_input, dense_up, preferred_element_type=jnp.float32)
    dense_hidden = (jax.nn.silu(dense_gate_part) * dense_up_part).astype(jnp.bfloat16)
    dense_sum = jnp.dot(dense_hidden, dense_down, preferred_element_type=jnp.float32)
    padded_rows = jnp.concatenate([ffn_input, jnp.zeros((1, D), ffn_input.dtype)], axis=0)
    share_wide = widen(expert_shares)

    def expert_step(running, pieces_in):
        gate_mat, up_mat, down_mat, expert_index = pieces_in
        named_mask = expert_ids == expert_index
        picked = jnp.any(named_mask, axis=1)
        row_share = lax.optimization_barrier(jnp.sum(jnp.where(named_mask, share_wide, jnp.zeros_like(share_wide)), axis=1))
        row_share = jnp.concatenate([row_share, jnp.zeros((1,), row_share.dtype)])
        row_index = jnp.nonzero(picked, size=N_EP * CAP, fill_value=BATCH)[0].astype(jnp.int32)
        chosen_rows = padded_rows[row_index]
        gate_part = jnp.dot(chosen_rows, gate_mat, preferred_element_type=jnp.float32)
        up_part = jnp.dot(chosen_rows, up_mat, preferred_element_type=jnp.float32)
        expert_hidden = (jax.nn.silu(gate_part) * up_part).astype(jnp.bfloat16)
        expert_row = jnp.dot(expert_hidden, down_mat, preferred_element_type=jnp.float32).astype(jnp.bfloat16)
        running = running.at[row_index].add(row_share[row_index][:, None] * widen(expert_row))
        return (running, None)
    running = jnp.zeros((BATCH + 1, D), jnp.float32)
    running, _ = lax.scan(expert_step, running, (expert_gate, expert_up, expert_down, jnp.arange(EXPERTS, dtype=jnp.int32)))
    routed = running[:BATCH]
    return (mid_wide + routed + gate_value[:, None] * dense_sum).astype(jnp.bfloat16)
```

```python
import math
import jax
import jax.numpy as jnp
from jax import lax
from jax.experimental import pallas as pl
from jax.experimental.pallas import tpu as pltpu
from jax.sharding import Mesh
from jax.sharding import PartitionSpec as P

HD = 64
NORM_EPS = 1e-06
HEAD_EPS = 1e-05
THETA = 500000.0
LAMBDA_BASE = 0.2
F32 = jnp.float32
BF16 = jnp.bfloat16
BLOCKS = 4


def attention_body(
    lens, lam, tokens, mixer_gain, wq_hbm, wk_hbm, wv_hbm, head_gain, wo_hbm, keys_hbm, values_hbm,
    out, wq, wk, wv, wo, keys, values, qrows, scores, mixed, wsem, ksem, vsem,
):
    seqs, span, width = keys.shape
    heads = lam.shape[0]
    rows = seqs * heads
    block = span // BLOCKS
    weights = [
        pltpu.make_async_copy(src, dst, wsem.at[i])
        for i, (src, dst) in enumerate(((wk_hbm, wk), (wq_hbm, wq), (wv_hbm, wv), (wo_hbm, wo)))
    ]
    key_copies = [
        pltpu.make_async_copy(
            keys_hbm.at[:, pl.ds(b * block, block), :], keys.at[:, pl.ds(b * block, block), :], ksem.at[b]
        )
        for b in range(BLOCKS)
    ]
    value_copies = [
        pltpu.make_async_copy(
            values_hbm.at[pl.ds(b * 4, 4)], values.at[pl.ds(b * 4, 4)], vsem.at[b]
        )
        for b in range(seqs // 4)
    ]
    for copy in weights[:3] + key_copies + value_copies + weights[3:]:
        copy.start()

    resid = tokens[...].astype(F32)
    mean_square = jnp.mean(resid * resid, axis=-1, keepdims=True)
    normed = (resid * lax.rsqrt(mean_square + NORM_EPS) * mixer_gain[...]).astype(BF16)

    row = lax.broadcasted_iota(jnp.int32, (seqs, width), 0)
    lane = lax.broadcasted_iota(jnp.int32, (seqs, width), 1)
    position = jnp.zeros((seqs, width), jnp.int32)
    for s in range(seqs):
        position = jnp.where(row == s, lens[s], position)
    half = HD // 2
    frequency = jnp.exp((lane % half).astype(F32) * (-2.0 / HD * math.log(THETA)))
    angles = position.astype(F32) * frequency
    first = lane % HD < half
    cos_vals = jnp.cos(angles)
    sin_vals = jnp.sin(angles)
    sin_vals = jnp.where(first, -sin_vals, sin_vals)

    def rotate(tile):
        swapped = jnp.where(first, pltpu.roll(tile, width - half, 1), pltpu.roll(tile, half, 1))
        return (tile * cos_vals + swapped * sin_vals).astype(BF16).astype(F32)

    column = lax.broadcasted_iota(jnp.int32, (1, width), 1)
    owner = column % rows // heads
    limit = jnp.zeros((1, width), jnp.int32)
    for s in range(seqs):
        limit = jnp.where(owner == s, lens[s], limit)
    mult = jnp.ones((1, width), F32)
    for j in range(heads):
        mult = jnp.where(column == rows + column % rows // heads * heads + j, lam[j], mult)

    weights[0].wait()
    knew = rotate(jnp.dot(normed, wk[...], preferred_element_type=F32)).astype(BF16)
    weights[1].wait()
    query_raw = jnp.dot(normed, wq[...], preferred_element_type=F32)
    for j in range(heads):
        tile = rotate(query_raw[:, j * width : (j + 1) * width]) * HD ** (-0.5)
        qrows[pl.ds(j, seqs, stride=heads), :] = jnp.where(lane < HD, tile, 0.0)
        qrows[pl.ds(rows + j, seqs, stride=heads), :] = jnp.where(lane < HD, 0.0, tile)
    qcols = jnp.transpose(qrows[...])
    query = jnp.concatenate([jnp.where(owner == s, qcols, 0.0).astype(BF16) for s in range(seqs)], axis=0)
    weights[2].wait()
    vnew = jnp.dot(normed, wv[...], preferred_element_type=F32).astype(BF16).astype(F32)
    for j in range(heads):
        mixed[pl.ds(j, seqs, stride=heads), :] = vnew

    new_row = jnp.concatenate([knew[s : s + 1, :] for s in range(seqs)], axis=1)
    new_row = jnp.broadcast_to(new_row, (16, seqs * width))
    new_score = jnp.dot(new_row, query, preferred_element_type=F32)[:1]
    peak = new_score
    for b in range(BLOCKS):
        key_copies[b].wait()
        past = jnp.concatenate([keys[s, pl.ds(b * block, block), :] for s in range(seqs)], axis=1)
        score = jnp.dot(past, query, preferred_element_type=F32)
        place = lax.broadcasted_iota(jnp.int32, (block, width), 0) + b * block
        score = jnp.where(place < limit, score, -jnp.inf)
        scores[pl.ds(b * block, block), :] = score
        peak = jnp.maximum(peak, jnp.max(score, axis=0, keepdims=True))
    expo = jnp.exp(scores[...] - peak)
    expo_new = jnp.exp(new_score - peak)
    factor = mult / (jnp.sum(expo, axis=0, keepdims=True) + expo_new)
    scaled = expo * factor
    weight = jnp.transpose(scaled - pltpu.roll(scaled, rows, 1))[:rows].astype(BF16)
    scaled_new = jnp.broadcast_to(expo_new * factor, (width, width))
    weight_new = jnp.transpose(scaled_new - pltpu.roll(scaled_new, rows, 1))[:rows].astype(BF16).astype(F32)
    pair = 8 // heads
    part = lax.broadcasted_iota(jnp.int32, (8, width), 0) // heads
    for g in range(seqs // pair):
        group = jnp.zeros((8, width), F32)
        for i in range(pair):
            s = g * pair + i
            if s % 4 == 0:
                value_copies[s // 4].wait()
            own = jnp.dot(weight[g * 8 : g * 8 + 8], values[s], preferred_element_type=F32)
            group = jnp.where(part == i, own, group)
        where = pl.ds(g * 8, 8)
        mixed[where, :] = group + weight_new[g * 8 : g * 8 + 8] * mixed[where, :]
    mix = mixed[...]
    mix_square = jnp.mean(mix * mix, axis=-1, keepdims=True)
    mixed[...] = mix * lax.rsqrt(mix_square + HEAD_EPS) * head_gain[...] * (1.0 - LAMBDA_BASE)
    head_out = jnp.concatenate([mixed[pl.ds(j, seqs, stride=heads), :] for j in range(heads)], axis=1)
    weights[3].wait()
    out[...] = jnp.dot(head_out.astype(BF16), wo[...], preferred_element_type=F32)


def attention(lens, lam, tokens, mixer_gain, wq, wk, wv, head_gain, wo, cache_keys, cache_values):
    seqs, model_width = tokens.shape
    span, width = cache_keys.shape[1:]
    heads = lam.shape[0]
    smem = pl.BlockSpec(memory_space=pltpu.SMEM)
    vmem = pl.BlockSpec(memory_space=pltpu.VMEM)
    hbm = pl.BlockSpec(memory_space=pltpu.HBM)
    return pl.pallas_call(
        attention_body,
        out_shape=jax.ShapeDtypeStruct((seqs, model_width), F32),
        in_specs=[smem, smem, vmem, vmem, hbm, hbm, hbm, vmem, hbm, hbm, hbm],
        out_specs=vmem,
        scratch_shapes=[
            pltpu.VMEM(wq.shape, BF16),
            pltpu.VMEM(wk.shape, BF16),
            pltpu.VMEM(wv.shape, BF16),
            pltpu.VMEM(wo.shape, BF16),
            pltpu.VMEM((seqs, span, width), BF16),
            pltpu.VMEM((seqs, span, width), BF16),
            pltpu.VMEM((2 * seqs * heads, width), F32),
            pltpu.VMEM((span, width), F32),
            pltpu.VMEM((seqs * heads, width), F32),
            pltpu.SemaphoreType.DMA((4,)),
            pltpu.SemaphoreType.DMA((BLOCKS,)),
            pltpu.SemaphoreType.DMA((4,)),
        ],
        compiler_params=pltpu.CompilerParams(vmem_limit_bytes=62 * 1024 * 1024),
        cost_estimate=pl.CostEstimate(flops=10**9, bytes_accessed=12 * 1024 * 1024, transcendentals=10**6),
        name="attention",
    )(lens, lam, tokens, mixer_gain, wq, wk, wv, head_gain, wo, cache_keys, cache_values)


EP = ("zh", "zl", "yh", "yl", "xh", "xl")
SMEM = pl.BlockSpec(memory_space=pltpu.SMEM)
VMEM = pl.BlockSpec(memory_space=pltpu.VMEM)


def call(body, name, out_shape, in_specs, scratch=(), flops=10**8):
    return pl.pallas_call(
        body,
        out_shape=out_shape,
        in_specs=in_specs,
        out_specs=jax.tree.map(lambda _: VMEM, out_shape),
        scratch_shapes=list(scratch),
        compiler_params=pltpu.CompilerParams(vmem_limit_bytes=24 * 1024 * 1024),
        cost_estimate=pl.CostEstimate(flops=flops, bytes_accessed=2 * 1024 * 1024, transcendentals=10**5),
        name=name,
    )


def pack_body(gate, up, down, out):
    units = down.shape[0]
    out[pl.ds(0, units), :] = jnp.transpose(gate[...].astype(F32)).astype(BF16)
    out[pl.ds(units, units), :] = jnp.transpose(up[...].astype(F32)).astype(BF16)
    out[pl.ds(2 * units, units), :] = down[...]


def mid_body(core, tokens, own, other, channel_gain, ids, shares, branch_gate, send, mid, pick, gate, slab):
    seqs, model_width = tokens.shape
    peers, lines, width = send.shape
    chunks = model_width // width
    summed = (tokens[...].astype(F32) + (own[...] + other[...])).astype(BF16)
    mid[...] = summed
    wide = summed.astype(F32)
    mean_square = jnp.mean(wide * wide, axis=-1, keepdims=True)
    ffn = (wide * lax.rsqrt(mean_square + NORM_EPS) * channel_gain[...]).astype(BF16)
    logit = jnp.sum(ffn.astype(F32) * branch_gate[...], axis=-1, keepdims=True)
    gate[...] = jnp.broadcast_to(jax.nn.sigmoid(logit), gate.shape)

    peer = lax.broadcasted_iota(jnp.int32, (seqs, peers), 1)
    row = lax.broadcasted_iota(jnp.int32, (seqs, peers), 0)
    share = jnp.zeros((seqs, peers), F32)
    picked = jnp.zeros((seqs, peers), F32)
    for k in range(ids.shape[1]):
        named = ids[:, k : k + 1] == peer
        picked = jnp.where(named, 1.0, picked)
        share = jnp.where(named, shares[:, k : k + 1].astype(F32), share)
    above = lax.broadcasted_iota(jnp.int32, (seqs, seqs), 0) >= lax.broadcasted_iota(jnp.int32, (seqs, seqs), 1)
    rank = jnp.dot(above.astype(BF16), picked.astype(BF16), preferred_element_type=F32)
    placed = (picked > 0.0) & (rank == (core[0] + 1).astype(F32))
    pick[...] = jnp.where(placed, share, 0.0).astype(BF16)
    dense = row == 2 * member(peer) + core[0]
    for r, chosen in enumerate((placed, dense)):
        lines_out = lax.dot_general(
            chosen.astype(F32).astype(BF16), ffn, (((0,), (0,)), ((), ())), preferred_element_type=F32
        )
        for k in range(chunks):
            slab[pl.ds(r * chunks + k, peers, stride=lines), :] = lines_out[:, k * width : (k + 1) * width]
    send[...] = slab[...].reshape(send.shape).astype(BF16)


def member(peer):
    return (peer // 16 % 2) * 4 + (peer // 4 % 2) * 2 + peer % 2


def unpack(slab, first, chunks, lines):
    peers = slab.shape[0] // lines
    return [slab[pl.ds(first + k, peers, stride=lines), :].astype(BF16) for k in range(chunks)]


def experts_body(
    core, arrived, gate_own, gate_other, up_own, up_other, down_own, down_other, dense_own, dense_other, out, slab
):
    peers, lines, width = arrived.shape
    chunks = lines // 2
    slab[...] = arrived[...].reshape(slab.shape).astype(F32)
    routed = jnp.concatenate(unpack(slab, 0, chunks, lines), axis=1)
    tokens = unpack(slab, chunks, chunks, lines)
    low, high = jnp.concatenate(tokens[: chunks // 2], axis=1), jnp.concatenate(tokens[chunks // 2 :], axis=1)
    is_first = core[0] == 0
    result = jnp.zeros((peers, chunks * width), F32)
    for w_gate, w_up, w_down in ((gate_own, up_own, down_own), (gate_other, up_other, down_other)):
        gate_part = jnp.dot(routed, w_gate[0], preferred_element_type=F32)
        up_part = jnp.dot(routed, w_up[0], preferred_element_type=F32)
        hidden = (jax.nn.silu(gate_part) * up_part).astype(BF16)
        result = result + jnp.dot(hidden, w_down[0], preferred_element_type=F32)
    for k in range(chunks):
        slab[pl.ds(k, peers, stride=lines), :] = result[:, k * width : (k + 1) * width]

    blocks, stacked, half_width = dense_own.shape
    units = stacked // 3

    def part(ref, i):
        return ref[:, i * units : (i + 1) * units, :].reshape(blocks * units, half_width)

    mine, theirs = jnp.where(is_first, low, high), jnp.where(is_first, high, low)

    def project(i):
        dims = (((1,), (1,)), ((), ()))
        return lax.dot_general(mine, part(dense_own, i), dims, preferred_element_type=F32) + lax.dot_general(
            theirs, part(dense_other, i), dims, preferred_element_type=F32
        )

    hidden = (jax.nn.silu(project(0)) * project(1)).astype(BF16)
    sum_own = jnp.dot(hidden, part(dense_own, 2), preferred_element_type=F32)
    sum_other = jnp.dot(hidden, part(dense_other, 2), preferred_element_type=F32)
    halves = (jnp.where(is_first, sum_own, sum_other), jnp.where(is_first, sum_other, sum_own))
    for h, value in enumerate(halves):
        for k in range(chunks // 2):
            where = pl.ds(chunks + h * chunks // 2 + k, peers, stride=lines)
            slab[where, :] = value[:, k * width : (k + 1) * width]
    out[...] = slab[...].reshape(out.shape).astype(BF16)


def combine_body(core, returned, pick, gate, mid, keep, send, slab):
    peers, lines, width = returned.shape
    chunks = lines // 2
    seqs = pick.shape[0]
    slab[...] = returned[...].reshape(slab.shape).astype(F32)
    peer = lax.broadcasted_iota(jnp.int32, (seqs, peers), 1)
    row = lax.broadcasted_iota(jnp.int32, (seqs, peers), 0)
    dense = (row == 2 * member(peer) + core[0]).astype(F32).astype(BF16)
    routed = jnp.dot(pick[...], jnp.concatenate(unpack(slab, 0, chunks, lines), axis=1), preferred_element_type=F32)
    branch = jnp.dot(dense, jnp.concatenate(unpack(slab, chunks, chunks, lines), axis=1), preferred_element_type=F32)
    total = routed + gate[:, :1] * branch
    half = chunks * width // 2
    is_first = core[0] == 0
    low, high = total[:, :half], total[:, half:]
    resid = mid[...].astype(F32)
    keep[...] = jnp.where(is_first, resid[:, :half] + low, resid[:, half:] + high)
    send[...] = jnp.where(is_first, high, low)


def swap(value, axis):
    return lax.ppermute(value, axis, [(0, 1), (1, 0)])


def shards(
    tokens, mixer_gain, query_weight, key_weight, value_weight, head_lambda, head_gain, out_weight,
    cache_keys, cache_values, seq_lengths, channel_gain, expert_ids, expert_shares,
    expert_gate, expert_up, expert_down, dense_gate, dense_up, dense_down, branch_gate,
):
    seqs, model_width = tokens.shape
    peers = lax.axis_size(EP)
    width = 2 * HD
    lines = 2 * model_width // width
    half = model_width // 2
    core = lax.axis_index("tp").astype(jnp.int32).reshape(1)
    sds = jax.ShapeDtypeStruct
    slab = pltpu.VMEM((peers * lines, width), F32)

    gate_other, up_other, down_other = (swap(w, "tp") for w in (expert_gate, expert_up, expert_down))
    units = dense_down.shape[0]
    packed = call(pack_body, "pack", sds((3 * units, half), BF16), [VMEM] * 3)(dense_gate, dense_up, dense_down)
    gathered = packed[None]
    for axis in ("xl", "yl", "zl"):
        gathered = jnp.concatenate([gathered, swap(gathered, axis)], axis=0)
    gathered_other = swap(gathered, "tp")

    own = attention(
        seq_lengths, head_lambda, tokens, mixer_gain.reshape(1, -1), query_weight, key_weight, value_weight,
        head_gain.reshape(1, -1), out_weight, cache_keys, cache_values,
    )
    other = swap(own, "tp")
    send, mid, pick, gate = call(
        mid_body,
        "mid",
        (
            sds((peers, lines, width), BF16),
            sds((seqs, model_width), BF16),
            sds((seqs, peers), BF16),
            sds((seqs, width), F32),
        ),
        [SMEM] + [VMEM] * 7,
        [slab],
    )(core, tokens, own, other, channel_gain.reshape(1, -1), expert_ids, expert_shares, branch_gate.reshape(1, -1))
    arrived = lax.all_to_all(send, EP, 0, 0, tiled=True)
    rows_out = call(experts_body, "experts", sds((peers, lines, width), BF16), [SMEM] + [VMEM] * 9, [slab])(
        core, arrived, expert_gate, gate_other, expert_up, up_other, expert_down, down_other, gathered, gathered_other
    )
    returned = lax.all_to_all(rows_out, EP, 0, 0, tiled=True)
    keep, give = call(
        combine_body, "combine", (sds((seqs, half), F32), sds((seqs, half), F32)), [SMEM] + [VMEM] * 4, [slab]
    )(core, returned, pick, gate, mid)
    return (keep + swap(give, "tp")).astype(BF16)


def solution(mesh):
    torus = Mesh(mesh.devices.reshape(4, 2, 2, 2, 2, 2, 2), (*EP, "tp"))
    return jax.shard_map(
        shards,
        mesh=torus,
        in_specs=(
            P(EP, None),
            P(),
            P(None, "tp"),
            P(None, "tp"),
            P(None, "tp"),
            P("tp"),
            P(),
            P("tp", None),
            P(EP, None, "tp"),
            P(EP, None, "tp"),
            P(EP),
            P(),
            P(EP, None),
            P(EP, None),
            P(EP, None, "tp"),
            P(EP, None, "tp"),
            P(EP, "tp", None),
            P("tp", EP),
            P("tp", EP),
            P(EP, "tp"),
            P(),
        ),
        out_specs=P(EP, "tp"),
        check_vma=False,
    )
```

```python
import math
import jax
import jax.numpy as jnp
from jax import lax
from jax.experimental import pallas as pl
from jax.experimental.pallas import tpu as pltpu
from jax.sharding import Mesh
from jax.sharding import PartitionSpec as P

HD = 64
NORM_EPS = 1e-06
HEAD_EPS = 1e-05
THETA = 500000.0
LAMBDA_BASE = 0.2
F32 = jnp.float32
BF16 = jnp.bfloat16
BLOCKS = 4


def attention_body(
    lens, lam, tokens, mixer_gain, wq_hbm, wk_hbm, wv_hbm, head_gain, wo_hbm, keys_hbm, values_hbm,
    out, wq, wk, wv, wo, keys, values, qrows, scores, mixed, wsem, ksem, vsem,
):
    seqs, span, width = keys.shape
    heads = lam.shape[0]
    rows = seqs * heads
    block = span // BLOCKS
    half_span, half_seqs = span // 2, seqs // 2
    weights = [
        pltpu.make_async_copy(src, dst, wsem.at[i])
        for i, (src, dst) in enumerate(((wk_hbm, wk), (wq_hbm, wq), (wv_hbm, wv), (wo_hbm, wo)))
    ]
    key_copies = [
        pltpu.make_async_copy(
            keys_hbm.at[:, pl.ds(b * half_span, half_span), :], keys.at[:, pl.ds(b * half_span, half_span), :], ksem.at[b]
        )
        for b in range(2)
    ]
    value_copies = [
        pltpu.make_async_copy(
            values_hbm.at[pl.ds(b * half_seqs, half_seqs)], values.at[pl.ds(b * half_seqs, half_seqs)], vsem.at[b]
        )
        for b in range(2)
    ]
    for copy in weights[:3] + key_copies:
        copy.start()

    resid = tokens[...].astype(F32)
    mean_square = jnp.mean(resid * resid, axis=-1, keepdims=True)
    normed = (resid * lax.rsqrt(mean_square + NORM_EPS) * mixer_gain[...]).astype(BF16)

    row = lax.broadcasted_iota(jnp.int32, (seqs, width), 0)
    lane = lax.broadcasted_iota(jnp.int32, (seqs, width), 1)
    position = jnp.zeros((seqs, width), jnp.int32)
    for s in range(seqs):
        position = jnp.where(row == s, lens[s], position)
    half = HD // 2
    frequency = jnp.exp((lane % half).astype(F32) * (-2.0 / HD * math.log(THETA)))
    angles = position.astype(F32) * frequency
    first = lane % HD < half
    cos_vals = jnp.cos(angles)
    sin_vals = jnp.sin(angles)
    sin_vals = jnp.where(first, -sin_vals, sin_vals)

    def rotate(tile):
        swapped = jnp.where(first, pltpu.roll(tile, width - half, 1), pltpu.roll(tile, half, 1))
        return (tile * cos_vals + swapped * sin_vals).astype(BF16).astype(F32)

    column = lax.broadcasted_iota(jnp.int32, (1, width), 1)
    owner = column % rows // heads
    limit = jnp.zeros((1, width), jnp.int32)
    for s in range(seqs):
        limit = jnp.where(owner == s, lens[s], limit)
    mult = jnp.ones((1, width), F32)
    for j in range(heads):
        mult = jnp.where(column == rows + column % rows // heads * heads + j, lam[j], mult)

    weights[0].wait()
    knew = rotate(jnp.dot(normed, wk[...], preferred_element_type=F32)).astype(BF16)
    weights[1].wait()
    query_raw = jnp.dot(normed, wq[...], preferred_element_type=F32)
    for j in range(heads):
        tile = rotate(query_raw[:, j * width : (j + 1) * width]) * HD ** (-0.5)
        qrows[pl.ds(j, seqs, stride=heads), :] = jnp.where(lane < HD, tile, 0.0)
        qrows[pl.ds(rows + j, seqs, stride=heads), :] = jnp.where(lane < HD, 0.0, tile)
    qcols = jnp.transpose(qrows[...])
    query = jnp.concatenate([jnp.where(owner == s, qcols, 0.0).astype(BF16) for s in range(seqs)], axis=0)
    weights[2].wait()
    vnew = jnp.dot(normed, wv[...], preferred_element_type=F32).astype(BF16).astype(F32)
    for j in range(heads):
        mixed[pl.ds(j, seqs, stride=heads), :] = vnew

    new_row = jnp.concatenate([knew[s : s + 1, :] for s in range(seqs)], axis=1)
    new_row = jnp.broadcast_to(new_row, (16, seqs * width))
    new_score = jnp.dot(new_row, query, preferred_element_type=F32)[:1]
    peak = new_score
    for b in range(BLOCKS):
        if b * block % half_span == 0:
            key_copies[b * block // half_span].wait()
        past = jnp.concatenate([keys[s, pl.ds(b * block, block), :] for s in range(seqs)], axis=1)
        score = jnp.dot(past, query, preferred_element_type=F32)
        if b == 0:
            for copy in value_copies + weights[3:]:
                copy.start()
        place = lax.broadcasted_iota(jnp.int32, (block, width), 0) + b * block
        score = jnp.where(place < limit, score, -jnp.inf)
        scores[pl.ds(b * block, block), :] = score
        peak = jnp.maximum(peak, jnp.max(score, axis=0, keepdims=True))
    expo = jnp.exp(scores[...] - peak)
    expo_new = jnp.exp(new_score - peak)
    factor = mult / (jnp.sum(expo, axis=0, keepdims=True) + expo_new)
    scaled = expo * factor
    weight = jnp.transpose(scaled - pltpu.roll(scaled, rows, 1))[:rows].astype(BF16)
    scaled_new = jnp.broadcast_to(expo_new * factor, (width, width))
    weight_new = jnp.transpose(scaled_new - pltpu.roll(scaled_new, rows, 1))[:rows].astype(BF16).astype(F32)
    pair = 8 // heads
    part = lax.broadcasted_iota(jnp.int32, (8, width), 0) // heads
    for g in range(seqs // pair):
        group = jnp.zeros((8, width), F32)
        for i in range(pair):
            s = g * pair + i
            if s % half_seqs == 0:
                value_copies[s // half_seqs].wait()
            own = jnp.dot(weight[g * 8 : g * 8 + 8], values[s], preferred_element_type=F32)
            group = jnp.where(part == i, own, group)
        where = pl.ds(g * 8, 8)
        mixed[where, :] = group + weight_new[g * 8 : g * 8 + 8] * mixed[where, :]
    mix = mixed[...]
    mix_square = jnp.mean(mix * mix, axis=-1, keepdims=True)
    mixed[...] = mix * lax.rsqrt(mix_square + HEAD_EPS) * head_gain[...] * (1.0 - LAMBDA_BASE)
    head_out = jnp.concatenate([mixed[pl.ds(j, seqs, stride=heads), :] for j in range(heads)], axis=1)
    weights[3].wait()
    out[...] = jnp.dot(head_out.astype(BF16), wo[...], preferred_element_type=F32)


def attention(lens, lam, tokens, mixer_gain, wq, wk, wv, head_gain, wo, cache_keys, cache_values):
    seqs, model_width = tokens.shape
    span, width = cache_keys.shape[1:]
    heads = lam.shape[0]
    smem = pl.BlockSpec(memory_space=pltpu.SMEM)
    vmem = pl.BlockSpec(memory_space=pltpu.VMEM)
    hbm = pl.BlockSpec(memory_space=pltpu.HBM)
    operands = (lens, lam, tokens, mixer_gain, wq, wk, wv, head_gain, wo, cache_keys, cache_values)
    operands = [pltpu.with_memory_space_constraint(x, pltpu.HBM) for x in operands]
    return pl.pallas_call(
        attention_body,
        out_shape=pltpu.VMEM((seqs, model_width), F32),
        in_specs=[smem, smem, vmem, vmem, hbm, hbm, hbm, vmem, hbm, hbm, hbm],
        out_specs=vmem,
        scratch_shapes=[
            pltpu.VMEM(wq.shape, BF16),
            pltpu.VMEM(wk.shape, BF16),
            pltpu.VMEM(wv.shape, BF16),
            pltpu.VMEM(wo.shape, BF16),
            pltpu.VMEM((seqs, span, width), BF16),
            pltpu.VMEM((seqs, span, width), BF16),
            pltpu.VMEM((2 * seqs * heads, width), F32),
            pltpu.VMEM((span, width), F32),
            pltpu.VMEM((seqs * heads, width), F32),
            pltpu.SemaphoreType.DMA((4,)),
            pltpu.SemaphoreType.DMA((2,)),
            pltpu.SemaphoreType.DMA((2,)),
        ],
        compiler_params=pltpu.CompilerParams(vmem_limit_bytes=20 * 1024 * 1024),
        cost_estimate=pl.CostEstimate(flops=10**9, bytes_accessed=12 * 1024 * 1024, transcendentals=10**6),
        name="attention",
    )(*operands)


EP = ("zh", "zl", "yh", "yl", "xh", "xl")
CUBE = ("zl", "yl", "xl")
SMEM = pl.BlockSpec(memory_space=pltpu.SMEM)
VMEM = pl.BlockSpec(memory_space=pltpu.VMEM)


def call(body, name, out_shape, in_specs, scratch=(), flops=10**8):
    return pl.pallas_call(
        body,
        out_shape=out_shape,
        in_specs=in_specs,
        out_specs=jax.tree.map(lambda _: VMEM, out_shape),
        scratch_shapes=list(scratch),
        compiler_params=pltpu.CompilerParams(vmem_limit_bytes=24 * 1024 * 1024),
        cost_estimate=pl.CostEstimate(flops=flops, bytes_accessed=2 * 1024 * 1024, transcendentals=10**5),
        name=name,
    )


def mid_body(core, tokens, own, other, channel_gain, ids, shares, branch_gate, send, mid, pick, gate, slab):
    seqs, model_width = tokens.shape
    peers, lines, width = send.shape
    chunks = model_width // width
    summed = (tokens[...].astype(F32) + (own[...] + other[...])).astype(BF16)
    mid[...] = summed
    wide = summed.astype(F32)
    mean_square = jnp.mean(wide * wide, axis=-1, keepdims=True)
    ffn = (wide * lax.rsqrt(mean_square + NORM_EPS) * channel_gain[...]).astype(BF16)
    logit = jnp.sum(ffn.astype(F32) * branch_gate[...], axis=-1, keepdims=True)
    gate[...] = jnp.broadcast_to(jax.nn.sigmoid(logit), gate.shape)

    peer = lax.broadcasted_iota(jnp.int32, (seqs, peers), 1)
    row = lax.broadcasted_iota(jnp.int32, (seqs, peers), 0)
    share = jnp.zeros((seqs, peers), F32)
    picked = jnp.zeros((seqs, peers), F32)
    for k in range(ids.shape[1]):
        named = ids[:, k : k + 1] == peer
        picked = jnp.where(named, 1.0, picked)
        share = jnp.where(named, shares[:, k : k + 1].astype(F32), share)
    above = lax.broadcasted_iota(jnp.int32, (seqs, seqs), 0) >= lax.broadcasted_iota(jnp.int32, (seqs, seqs), 1)
    rank = jnp.dot(above.astype(BF16), picked.astype(BF16), preferred_element_type=F32)
    placed = (picked > 0.0) & (rank == (core[0] + 1).astype(F32))
    pick[...] = jnp.where(placed, share, 0.0).astype(BF16)
    dense = row == 2 * member(peer) + core[0]
    for r, chosen in enumerate((placed, dense)):
        lines_out = lax.dot_general(
            chosen.astype(F32).astype(BF16), ffn, (((0,), (0,)), ((), ())), preferred_element_type=F32
        )
        for k in range(chunks):
            slab[pl.ds(r * chunks + k, peers, stride=lines), :] = lines_out[:, k * width : (k + 1) * width]
    send[...] = slab[...].reshape(send.shape).astype(BF16)


def member(peer):
    return (peer // 16 % 2) * 4 + (peer // 4 % 2) * 2 + peer % 2


def unpack(slab, first, chunks, lines):
    peers = slab.shape[0] // lines
    return [slab[pl.ds(first + k, peers, stride=lines), :].astype(BF16) for k in range(chunks)]


def experts_body(
    core, arrived, gate_own, gate_other, up_own, up_other, dense_own, dense_other, down_own, down_other, out, slab,
    downs, sems,
):
    down_copies = [
        pltpu.make_async_copy(src, downs.at[pl.ds(i, 1)], sems.at[i]) for i, src in enumerate((down_own, down_other))
    ]
    for copy in down_copies:
        copy.start()
    peers, lines, width = arrived.shape
    chunks = lines // 2
    slab[...] = arrived[...].reshape(slab.shape).astype(F32)
    routed = jnp.concatenate(unpack(slab, 0, chunks, lines), axis=1)
    tokens = unpack(slab, chunks, chunks, lines)
    low, high = jnp.concatenate(tokens[: chunks // 2], axis=1), jnp.concatenate(tokens[chunks // 2 :], axis=1)
    is_first = core[0] == 0
    result = jnp.zeros((peers, chunks * width), F32)
    for i, (w_gate, w_up) in enumerate(((gate_own, up_own), (gate_other, up_other))):
        gate_part = jnp.dot(routed, w_gate[0], preferred_element_type=F32)
        up_part = jnp.dot(routed, w_up[0], preferred_element_type=F32)
        hidden = (jax.nn.silu(gate_part) * up_part).astype(BF16)
        down_copies[i].wait()
        result = result + jnp.dot(hidden, downs[i], preferred_element_type=F32)
    for k in range(chunks):
        slab[pl.ds(k, peers, stride=lines), :] = result[:, k * width : (k + 1) * width]

    blocks, stacked, half_width = dense_own.shape
    units = stacked // 3

    def part(ref, i):
        return ref[:, i * units : (i + 1) * units, :].reshape(blocks * units, half_width)

    mine, theirs = jnp.where(is_first, low, high), jnp.where(is_first, high, low)

    def project(i):
        dims = (((1,), (1,)), ((), ()))
        return lax.dot_general(mine, part(dense_own, i), dims, preferred_element_type=F32) + lax.dot_general(
            theirs, part(dense_other, i), dims, preferred_element_type=F32
        )

    hidden = (jax.nn.silu(project(0)) * project(1)).astype(BF16)
    sum_own = jnp.dot(hidden, part(dense_own, 2), preferred_element_type=F32)
    sum_other = jnp.dot(hidden, part(dense_other, 2), preferred_element_type=F32)
    halves = (jnp.where(is_first, sum_own, sum_other), jnp.where(is_first, sum_other, sum_own))
    for h, value in enumerate(halves):
        for k in range(chunks // 2):
            where = pl.ds(chunks + h * chunks // 2 + k, peers, stride=lines)
            slab[where, :] = value[:, k * width : (k + 1) * width]
    out[...] = slab[...].reshape(out.shape).astype(BF16)


def combine_body(core, returned, pick, gate, mid, keep, send, slab):
    peers, lines, width = returned.shape
    chunks = lines // 2
    seqs = pick.shape[0]
    slab[...] = returned[...].reshape(slab.shape).astype(F32)
    peer = lax.broadcasted_iota(jnp.int32, (seqs, peers), 1)
    row = lax.broadcasted_iota(jnp.int32, (seqs, peers), 0)
    dense = (row == 2 * member(peer) + core[0]).astype(F32).astype(BF16)
    routed = jnp.dot(pick[...], jnp.concatenate(unpack(slab, 0, chunks, lines), axis=1), preferred_element_type=F32)
    branch = jnp.dot(dense, jnp.concatenate(unpack(slab, chunks, chunks, lines), axis=1), preferred_element_type=F32)
    total = routed + gate[:, :1] * branch
    half = chunks * width // 2
    is_first = core[0] == 0
    low, high = total[:, :half], total[:, half:]
    resid = mid[...].astype(F32)
    keep[...] = jnp.where(is_first, resid[:, :half] + low, resid[:, half:] + high)
    send[...] = jnp.where(is_first, high, low)


def swap(value, axis):
    return lax.ppermute(value, axis, [(0, 1), (1, 0)])


def shards(
    tokens, mixer_gain, query_weight, key_weight, value_weight, head_lambda, head_gain, out_weight,
    cache_keys, cache_values, seq_lengths, channel_gain, expert_ids, expert_shares,
    expert_gate, expert_up, expert_down, dense_gate, dense_up, dense_down, branch_gate,
):
    seqs, model_width = tokens.shape
    peers = lax.axis_size(EP)
    width = 2 * HD
    lines = 2 * model_width // width
    half = model_width // 2
    core = lax.axis_index("tp").astype(jnp.int32).reshape(1)
    sds = jax.ShapeDtypeStruct
    slab = pltpu.VMEM((peers * lines, width), F32)

    packed = jnp.concatenate([dense_gate.T, dense_up.T, dense_down], axis=0)
    copies = jnp.broadcast_to(packed[None], (2 ** len(CUBE), *packed.shape))
    gathered = lax.all_to_all(copies, CUBE, 0, 0, tiled=True)
    gate_other, up_other, down_other = (swap(w, "tp") for w in (expert_gate, expert_up, expert_down))

    own = attention(
        seq_lengths, head_lambda, tokens, mixer_gain.reshape(1, -1), query_weight, key_weight, value_weight,
        head_gain.reshape(1, -1), out_weight, cache_keys, cache_values,
    )
    other = swap(own, "tp")
    gathered_other = swap(gathered, "tp")
    send, mid, pick, gate = call(
        mid_body,
        "mid",
        (
            sds((peers, lines, width), BF16),
            sds((seqs, model_width), BF16),
            sds((seqs, peers), BF16),
            sds((seqs, width), F32),
        ),
        [SMEM] + [VMEM] * 7,
        [slab],
    )(core, tokens, own, other, channel_gain.reshape(1, -1), expert_ids, expert_shares, branch_gate.reshape(1, -1))
    arrived = lax.all_to_all(send, EP, 0, 0, tiled=True)
    pinned = [pltpu.with_memory_space_constraint(w, pltpu.HBM) for w in (expert_down, down_other)]
    rows_out = call(
        experts_body,
        "experts",
        sds((peers, lines, width), BF16),
        [SMEM] + [VMEM] * 7 + [pl.BlockSpec(memory_space=pltpu.HBM)] * 2,
        [slab, pltpu.VMEM((2, *expert_down.shape[1:]), BF16), pltpu.SemaphoreType.DMA((2,))],
    )(core, arrived, expert_gate, gate_other, expert_up, up_other, gathered, gathered_other, *pinned)
    returned = lax.all_to_all(rows_out, EP, 0, 0, tiled=True)
    keep, give = call(
        combine_body, "combine", (sds((seqs, half), F32), sds((seqs, half), F32)), [SMEM] + [VMEM] * 4, [slab]
    )(core, returned, pick, gate, mid)
    return (keep + swap(give, "tp")).astype(BF16)


def solution(mesh):
    torus = Mesh(mesh.devices.reshape(4, 2, 2, 2, 2, 2, 2), (*EP, "tp"))
    return jax.shard_map(
        shards,
        mesh=torus,
        in_specs=(
            P(EP, None),
            P(),
            P(None, "tp"),
            P(None, "tp"),
            P(None, "tp"),
            P("tp"),
            P(),
            P("tp", None),
            P(EP, None, "tp"),
            P(EP, None, "tp"),
            P(EP),
            P(),
            P(EP, None),
            P(EP, None),
            P(EP, None, "tp"),
            P(EP, None, "tp"),
            P(EP, "tp", None),
            P("tp", EP),
            P("tp", EP),
            P(EP, "tp"),
            P(),
        ),
        out_specs=P(EP, "tp"),
        check_vma=False,
    )
```

```python
import math
import jax
import jax.numpy as jnp
from jax import lax
from jax.experimental import pallas as pl
from jax.experimental.pallas import tpu as pltpu
from jax.sharding import Mesh
from jax.sharding import PartitionSpec as P

HD = 64
NORM_EPS = 1e-06
HEAD_EPS = 1e-05
THETA = 500000.0
LAMBDA_BASE = 0.2
F32 = jnp.float32
BF16 = jnp.bfloat16
BLOCKS = 4


def attention_body(
    lens_hbm, lam_hbm, tokens_hbm, mixer_hbm, wq_hbm, wk_hbm, wv_hbm, head_gain_hbm, wo_hbm, keys_hbm, values_hbm, out,
    lens, lam, tokens, mixer_gain, head_gain, wq, wk, wv, wo, keys, values, qrows, scores, mixed, ssem, wsem, ksem, vsem,
):
    seqs, span, width = keys.shape
    heads = lam.shape[0]
    rows = seqs * heads
    block = span // BLOCKS
    half_span, half_seqs = span // 2, seqs // 2
    weights = [
        pltpu.make_async_copy(src, dst, wsem.at[i])
        for i, (src, dst) in enumerate(((wk_hbm, wk), (wq_hbm, wq), (wv_hbm, wv), (wo_hbm, wo)))
    ]
    key_copies = [
        pltpu.make_async_copy(
            keys_hbm.at[:, pl.ds(b * half_span, half_span), :], keys.at[:, pl.ds(b * half_span, half_span), :], ksem.at[b]
        )
        for b in range(2)
    ]
    value_copies = [
        pltpu.make_async_copy(
            values_hbm.at[pl.ds(b * half_seqs, half_seqs)], values.at[pl.ds(b * half_seqs, half_seqs)], vsem.at[b]
        )
        for b in range(2)
    ]
    small = [
        pltpu.make_async_copy(src, dst, ssem.at[i])
        for i, (src, dst) in enumerate(
            (
                (tokens_hbm, tokens), (mixer_hbm, mixer_gain), (lens_hbm, lens), (lam_hbm, lam),
                (head_gain_hbm, head_gain),
            )
        )
    ]
    for copy in small + weights[:3] + key_copies:
        copy.start()
    for copy in small[:2]:
        copy.wait()

    resid = tokens[...].astype(F32)
    mean_square = jnp.mean(resid * resid, axis=-1, keepdims=True)
    normed = (resid * lax.rsqrt(mean_square + NORM_EPS) * mixer_gain[...]).astype(BF16)

    weights[0].wait()
    key_raw = jnp.dot(normed, wk[...], preferred_element_type=F32)
    weights[1].wait()
    query_raw = jnp.dot(normed, wq[...], preferred_element_type=F32)
    for copy in value_copies + weights[3:]:
        copy.start()
    for copy in small[2:]:
        copy.wait()

    row = lax.broadcasted_iota(jnp.int32, (seqs, width), 0)
    lane = lax.broadcasted_iota(jnp.int32, (seqs, width), 1)
    position = jnp.zeros((seqs, width), jnp.int32)
    for s in range(seqs):
        position = jnp.where(row == s, lens[s], position)
    half = HD // 2
    frequency = jnp.exp((lane % half).astype(F32) * (-2.0 / HD * math.log(THETA)))
    angles = position.astype(F32) * frequency
    first = lane % HD < half
    cos_vals = jnp.cos(angles)
    sin_vals = jnp.sin(angles)
    sin_vals = jnp.where(first, -sin_vals, sin_vals)

    def rotate(tile):
        swapped = jnp.where(first, pltpu.roll(tile, width - half, 1), pltpu.roll(tile, half, 1))
        return (tile * cos_vals + swapped * sin_vals).astype(BF16).astype(F32)

    column = lax.broadcasted_iota(jnp.int32, (1, width), 1)
    owner = column % rows // heads
    limit = jnp.zeros((1, width), jnp.int32)
    for s in range(seqs):
        limit = jnp.where(owner == s, lens[s], limit)
    mult = jnp.ones((1, width), F32)
    for j in range(heads):
        mult = jnp.where(column == rows + column % rows // heads * heads + j, lam[j], mult)

    knew = rotate(key_raw).astype(BF16)
    for j in range(heads):
        tile = rotate(query_raw[:, j * width : (j + 1) * width]) * HD ** (-0.5)
        qrows[pl.ds(j, seqs, stride=heads), :] = jnp.where(lane < HD, tile, 0.0)
        qrows[pl.ds(rows + j, seqs, stride=heads), :] = jnp.where(lane < HD, 0.0, tile)
    qcols = jnp.transpose(qrows[...])
    query = jnp.concatenate([jnp.where(owner == s, qcols, 0.0).astype(BF16) for s in range(seqs)], axis=0)
    weights[2].wait()
    vnew = jnp.dot(normed, wv[...], preferred_element_type=F32).astype(BF16).astype(F32)
    for j in range(heads):
        mixed[pl.ds(j, seqs, stride=heads), :] = vnew

    new_row = jnp.concatenate([knew[s : s + 1, :] for s in range(seqs)], axis=1)
    new_row = jnp.broadcast_to(new_row, (16, seqs * width))
    new_score = jnp.dot(new_row, query, preferred_element_type=F32)[:1]
    peak = new_score
    for b in range(BLOCKS):
        if b * block % half_span == 0:
            key_copies[b * block // half_span].wait()
        past = jnp.concatenate([keys[s, pl.ds(b * block, block), :] for s in range(seqs)], axis=1)
        score = jnp.dot(past, query, preferred_element_type=F32)
        place = lax.broadcasted_iota(jnp.int32, (block, width), 0) + b * block
        score = jnp.where(place < limit, score, -jnp.inf)
        scores[pl.ds(b * block, block), :] = score
        peak = jnp.maximum(peak, jnp.max(score, axis=0, keepdims=True))
    expo = jnp.exp(scores[...] - peak)
    expo_new = jnp.exp(new_score - peak)
    factor = mult / (jnp.sum(expo, axis=0, keepdims=True) + expo_new)
    scaled = expo * factor
    weight = jnp.transpose(scaled - pltpu.roll(scaled, rows, 1))[:rows].astype(BF16)
    scaled_new = jnp.broadcast_to(expo_new * factor, (width, width))
    weight_new = jnp.transpose(scaled_new - pltpu.roll(scaled_new, rows, 1))[:rows].astype(BF16).astype(F32)
    pair = 8 // heads
    part = lax.broadcasted_iota(jnp.int32, (8, width), 0) // heads
    for g in range(seqs // pair):
        group = jnp.zeros((8, width), F32)
        for i in range(pair):
            s = g * pair + i
            if s % half_seqs == 0:
                value_copies[s // half_seqs].wait()
            own = jnp.dot(weight[g * 8 : g * 8 + 8], values[s], preferred_element_type=F32)
            group = jnp.where(part == i, own, group)
        where = pl.ds(g * 8, 8)
        mixed[where, :] = group + weight_new[g * 8 : g * 8 + 8] * mixed[where, :]
    mix = mixed[...]
    mix_square = jnp.mean(mix * mix, axis=-1, keepdims=True)
    mixed[...] = mix * lax.rsqrt(mix_square + HEAD_EPS) * head_gain[...] * (1.0 - LAMBDA_BASE)
    head_out = jnp.concatenate([mixed[pl.ds(j, seqs, stride=heads), :] for j in range(heads)], axis=1)
    weights[3].wait()
    out[...] = jnp.dot(head_out.astype(BF16), wo[...], preferred_element_type=F32)


def attention(lens, lam, tokens, mixer_gain, wq, wk, wv, head_gain, wo, cache_keys, cache_values):
    seqs, model_width = tokens.shape
    span, width = cache_keys.shape[1:]
    heads = lam.shape[0]
    vmem = pl.BlockSpec(memory_space=pltpu.VMEM)
    hbm = pl.BlockSpec(memory_space=pltpu.HBM)
    operands = (lens, lam, tokens, mixer_gain, wq, wk, wv, head_gain, wo, cache_keys, cache_values)
    operands = [pltpu.with_memory_space_constraint(x, pltpu.HBM) for x in operands]
    return pl.pallas_call(
        attention_body,
        out_shape=pltpu.VMEM((seqs, model_width), F32),
        in_specs=[hbm] * 11,
        out_specs=vmem,
        scratch_shapes=[
            pltpu.SMEM(lens.shape, jnp.int32),
            pltpu.SMEM(lam.shape, F32),
            pltpu.VMEM(tokens.shape, BF16),
            pltpu.VMEM(mixer_gain.shape, F32),
            pltpu.VMEM(head_gain.shape, F32),
            pltpu.VMEM(wq.shape, BF16),
            pltpu.VMEM(wk.shape, BF16),
            pltpu.VMEM(wv.shape, BF16),
            pltpu.VMEM(wo.shape, BF16),
            pltpu.VMEM((seqs, span, width), BF16),
            pltpu.VMEM((seqs, span, width), BF16),
            pltpu.VMEM((2 * seqs * heads, width), F32),
            pltpu.VMEM((span, width), F32),
            pltpu.VMEM((seqs * heads, width), F32),
            pltpu.SemaphoreType.DMA((5,)),
            pltpu.SemaphoreType.DMA((4,)),
            pltpu.SemaphoreType.DMA((2,)),
            pltpu.SemaphoreType.DMA((2,)),
        ],
        compiler_params=pltpu.CompilerParams(vmem_limit_bytes=20 * 1024 * 1024),
        cost_estimate=pl.CostEstimate(flops=10**9, bytes_accessed=12 * 1024 * 1024, transcendentals=10**6),
        name="attention",
    )(*operands)


EP = ("zh", "zl", "yh", "yl", "xh", "xl")
SMEM = pl.BlockSpec(memory_space=pltpu.SMEM)
VMEM = pl.BlockSpec(memory_space=pltpu.VMEM)


def call(body, out_shape, in_specs, scratch=(), flops=10**8):
    return pl.pallas_call(
        body,
        out_shape=out_shape,
        in_specs=in_specs,
        out_specs=jax.tree.map(lambda _: VMEM, out_shape),
        scratch_shapes=list(scratch),
        compiler_params=pltpu.CompilerParams(vmem_limit_bytes=12 * 1024 * 1024),
        cost_estimate=pl.CostEstimate(flops=flops, bytes_accessed=2 * 1024 * 1024, transcendentals=10**5),
    )


def mid_body(core, tokens, own, other, channel_gain, ids, shares, branch_gate, send, mid, pick, gate, slab):
    seqs, model_width = tokens.shape
    peers, lines, width = send.shape
    chunks = model_width // width
    summed = (tokens[...].astype(F32) + (own[...] + other[...])).astype(BF16)
    mid[...] = summed
    wide = summed.astype(F32)
    mean_square = jnp.mean(wide * wide, axis=-1, keepdims=True)
    ffn = (wide * lax.rsqrt(mean_square + NORM_EPS) * channel_gain[...]).astype(BF16)
    logit = jnp.sum(ffn.astype(F32) * branch_gate[...], axis=-1, keepdims=True)
    gate[...] = jnp.broadcast_to(jax.nn.sigmoid(logit), gate.shape)

    peer = lax.broadcasted_iota(jnp.int32, (seqs, peers), 1)
    row = lax.broadcasted_iota(jnp.int32, (seqs, peers), 0)
    share = jnp.zeros((seqs, peers), F32)
    picked = jnp.zeros((seqs, peers), F32)
    for k in range(ids.shape[1]):
        named = ids[:, k : k + 1] == peer
        picked = jnp.where(named, 1.0, picked)
        share = jnp.where(named, shares[:, k : k + 1].astype(F32), share)
    above = lax.broadcasted_iota(jnp.int32, (seqs, seqs), 0) >= lax.broadcasted_iota(jnp.int32, (seqs, seqs), 1)
    rank = jnp.dot(above.astype(BF16), picked.astype(BF16), preferred_element_type=F32)
    placed = (picked > 0.0) & (rank == (core[0] + 1).astype(F32))
    pick[...] = jnp.where(placed, share, 0.0).astype(BF16)
    dense = row == 2 * member(peer) + core[0]
    for r, chosen in enumerate((placed, dense)):
        lines_out = lax.dot_general(
            chosen.astype(F32).astype(BF16), ffn, (((0,), (0,)), ((), ())), preferred_element_type=F32
        )
        for k in range(chunks):
            slab[pl.ds(r * chunks + k, peers, stride=lines), :] = lines_out[:, k * width : (k + 1) * width]
    send[...] = slab[...].reshape(send.shape).astype(BF16)


def member(peer):
    return (peer // 16 % 2) * 4 + (peer // 4 % 2) * 2 + peer % 2


def unpack(slab, first, chunks, lines):
    peers = slab.shape[0] // lines
    return [slab[pl.ds(first + k, peers, stride=lines), :].astype(BF16) for k in range(chunks)]


def experts_body(
    core, arrived, gate_own, gate_other, up_own, up_other, dense_own, dense_other, down_own, down_other, out, slab,
    down_late, sem,
):
    late = pltpu.make_async_copy(down_other, down_late, sem)
    late.start()
    peers, lines, width = arrived.shape
    chunks = lines // 2
    slab[...] = arrived[...].reshape(slab.shape).astype(F32)
    routed = jnp.concatenate(unpack(slab, 0, chunks, lines), axis=1)
    tokens = unpack(slab, chunks, chunks, lines)
    low, high = jnp.concatenate(tokens[: chunks // 2], axis=1), jnp.concatenate(tokens[chunks // 2 :], axis=1)
    is_first = core[0] == 0
    blocks, stacked, half_width = dense_own.shape
    units = stacked // 3

    def part(ref, i):
        return ref[:, i * units : (i + 1) * units, :].reshape(blocks * units, half_width)

    mine, theirs = jnp.where(is_first, low, high), jnp.where(is_first, high, low)

    def project(i):
        dims = (((1,), (1,)), ((), ()))
        return lax.dot_general(mine, part(dense_own, i), dims, preferred_element_type=F32) + lax.dot_general(
            theirs, part(dense_other, i), dims, preferred_element_type=F32
        )

    hidden = (jax.nn.silu(project(0)) * project(1)).astype(BF16)
    sum_own = jnp.dot(hidden, part(dense_own, 2), preferred_element_type=F32)
    sum_other = jnp.dot(hidden, part(dense_other, 2), preferred_element_type=F32)
    halves = (jnp.where(is_first, sum_own, sum_other), jnp.where(is_first, sum_other, sum_own))
    for h, value in enumerate(halves):
        for k in range(chunks // 2):
            where = pl.ds(chunks + h * chunks // 2 + k, peers, stride=lines)
            slab[where, :] = value[:, k * width : (k + 1) * width]
    result = jnp.zeros((peers, chunks * width), F32)
    for w_gate, w_up, w_down in ((gate_own, up_own, down_own), (gate_other, up_other, down_late)):
        gate_part = jnp.dot(routed, w_gate[0], preferred_element_type=F32)
        up_part = jnp.dot(routed, w_up[0], preferred_element_type=F32)
        hidden = (jax.nn.silu(gate_part) * up_part).astype(BF16)
        if w_down is down_late:
            late.wait()
        result = result + jnp.dot(hidden, w_down[0], preferred_element_type=F32)
    for k in range(chunks):
        slab[pl.ds(k, peers, stride=lines), :] = result[:, k * width : (k + 1) * width]
    out[...] = slab[...].reshape(out.shape).astype(BF16)


def combine_body(core, returned, pick, gate, mid, keep, send, slab):
    peers, lines, width = returned.shape
    chunks = lines // 2
    seqs = pick.shape[0]
    slab[...] = returned[...].reshape(slab.shape).astype(F32)
    peer = lax.broadcasted_iota(jnp.int32, (seqs, peers), 1)
    row = lax.broadcasted_iota(jnp.int32, (seqs, peers), 0)
    dense = (row == 2 * member(peer) + core[0]).astype(F32).astype(BF16)
    routed = jnp.dot(pick[...], jnp.concatenate(unpack(slab, 0, chunks, lines), axis=1), preferred_element_type=F32)
    branch = jnp.dot(dense, jnp.concatenate(unpack(slab, chunks, chunks, lines), axis=1), preferred_element_type=F32)
    total = routed + gate[:, :1] * branch
    half = chunks * width // 2
    is_first = core[0] == 0
    low, high = total[:, :half], total[:, half:]
    resid = mid[...].astype(F32)
    keep[...] = jnp.where(is_first, resid[:, :half] + low, resid[:, half:] + high)
    send[...] = jnp.where(is_first, high, low)


def swap(value, axis):
    return lax.ppermute(value, axis, [(0, 1), (1, 0)])


def layer(
    tokens, mixer_gain, query_weight, key_weight, value_weight, head_lambda, head_gain, out_weight,
    cache_keys, cache_values, seq_lengths, channel_gain, expert_ids, expert_shares,
    expert_gate, expert_up, expert_down, dense_gate, dense_up, dense_down, branch_gate,
):
    seqs, model_width = tokens.shape
    peers = lax.axis_size(EP)
    width = 2 * HD
    lines = 2 * model_width // width
    half = model_width // 2
    core = lax.axis_index("tp").astype(jnp.int32).reshape(1)
    sds = jax.ShapeDtypeStruct
    slab = pltpu.VMEM((peers * lines, width), F32)

    gate_other, up_other, down_other = (swap(w, "tp") for w in (expert_gate, expert_up, expert_down))

    first = jnp.concatenate([dense_gate.T, dense_up.T, dense_down], axis=0)[None]
    second = swap(first, "zl")
    own = attention(
        seq_lengths, head_lambda, tokens, mixer_gain.reshape(1, -1), query_weight, key_weight, value_weight,
        head_gain.reshape(1, -1), out_weight, cache_keys, cache_values,
    )
    other = swap(own, "tp")
    pair = jnp.concatenate([first, second], axis=0)
    pair_y = swap(pair, "yl")
    pair_x = swap(pair, "xl")
    cut_y, cut_x = pair_y[:1], pair_x[1:]
    corner_x = swap(cut_y, "xl")
    corner_y = swap(cut_x, "yl")
    gathered = jnp.concatenate([pair, pair_y, pair_x, corner_x, corner_y], axis=0)
    gathered_other = swap(gathered, "tp")
    middle = call(
        mid_body,
        (
            sds((peers, lines, width), BF16),
            sds((seqs, model_width), BF16),
            sds((seqs, peers), BF16),
            sds((seqs, width), F32),
        ),
        [SMEM] + [VMEM] * 7,
        [slab],
    )
    send, mid, pick, gate = middle(
        core, tokens, own, other, channel_gain.reshape(1, -1), expert_ids, expert_shares, branch_gate.reshape(1, -1)
    )
    arrived = lax.all_to_all(send, EP, 0, 0, tiled=True)
    down_other = pltpu.with_memory_space_constraint(down_other, pltpu.HBM)
    rows_out = call(
        experts_body,
        sds((peers, lines, width), BF16),
        [SMEM] + [VMEM] * 8 + [pl.BlockSpec(memory_space=pltpu.HBM)],
        [slab, pltpu.VMEM(expert_down.shape, BF16), pltpu.SemaphoreType.DMA(())],
    )(core, arrived, expert_gate, gate_other, expert_up, up_other, gathered, gathered_other, expert_down, down_other)
    returned = lax.all_to_all(rows_out, EP, 0, 0, tiled=True)
    keep, give = call(
        combine_body, (sds((seqs, half), F32), sds((seqs, half), F32)), [SMEM] + [VMEM] * 4, [slab]
    )(core, returned, pick, gate, mid)
    return (keep + swap(give, "tp")).astype(BF16)


def solution(mesh):
    torus = Mesh(mesh.devices.reshape(4, 2, 2, 2, 2, 2, 2), (*EP, "tp"))
    return jax.shard_map(
        layer,
        mesh=torus,
        in_specs=(
            P(EP, None),
            P(),
            P(None, "tp"),
            P(None, "tp"),
            P(None, "tp"),
            P("tp"),
            P(),
            P("tp", None),
            P(EP, None, "tp"),
            P(EP, None, "tp"),
            P(EP),
            P(),
            P(EP, None),
            P(EP, None),
            P(EP, None, "tp"),
            P(EP, None, "tp"),
            P(EP, "tp", None),
            P("tp", EP),
            P("tp", EP),
            P(EP, "tp"),
            P(),
        ),
        out_specs=P(EP, "tp"),
        check_vma=False,
    )
```

```python
import math
import jax
import jax.numpy as jnp
from jax import lax
from jax.experimental import pallas as pl
from jax.experimental.pallas import tpu as pltpu
from jax.sharding import Mesh
from jax.sharding import PartitionSpec as P

HD = 64
NORM_EPS = 1e-06
HEAD_EPS = 1e-05
THETA = 500000.0
LAMBDA_BASE = 0.2
F32 = jnp.float32
BF16 = jnp.bfloat16
BLOCKS = 4


def attention_body(
    lens_hbm, lam_hbm, tokens_hbm, mixer_hbm, wq_hbm, wk_hbm, wv_hbm, head_gain_hbm, wo_hbm, keys_hbm, values_hbm, out,
    lens, lam, tokens, mixer_gain, head_gain, wq, wk, wv, wo, keys, values, qrows, scores, mixed, ssem, wsem, ksem, vsem,
):
    seqs, span, width = keys.shape
    heads = lam.shape[0]
    rows = seqs * heads
    block = span // BLOCKS
    half_span, half_seqs = span // 2, seqs // 2
    weights = [
        pltpu.make_async_copy(src, dst, wsem.at[i])
        for i, (src, dst) in enumerate(((wk_hbm, wk), (wq_hbm, wq), (wv_hbm, wv), (wo_hbm, wo)))
    ]
    key_copies = [
        pltpu.make_async_copy(
            keys_hbm.at[:, pl.ds(b * half_span, half_span), :], keys.at[:, pl.ds(b * half_span, half_span), :], ksem.at[b]
        )
        for b in range(2)
    ]
    value_copies = [
        pltpu.make_async_copy(
            values_hbm.at[pl.ds(b * half_seqs, half_seqs)], values.at[pl.ds(b * half_seqs, half_seqs)], vsem.at[b]
        )
        for b in range(2)
    ]
    small = [
        pltpu.make_async_copy(src, dst, ssem.at[i])
        for i, (src, dst) in enumerate(
            (
                (tokens_hbm, tokens), (mixer_hbm, mixer_gain), (lens_hbm, lens), (lam_hbm, lam),
                (head_gain_hbm, head_gain),
            )
        )
    ]
    for copy in small + weights[:3] + key_copies:
        copy.start()
    for copy in small[:2]:
        copy.wait()

    resid = tokens[...].astype(F32)
    mean_square = jnp.mean(resid * resid, axis=-1, keepdims=True)
    normed = (resid * lax.rsqrt(mean_square + NORM_EPS) * mixer_gain[...]).astype(BF16)

    weights[0].wait()
    key_raw = jnp.dot(normed, wk[...], preferred_element_type=F32)
    weights[1].wait()
    query_raw = jnp.dot(normed, wq[...], preferred_element_type=F32)
    for copy in value_copies + weights[3:]:
        copy.start()
    for copy in small[2:]:
        copy.wait()

    row = lax.broadcasted_iota(jnp.int32, (seqs, width), 0)
    lane = lax.broadcasted_iota(jnp.int32, (seqs, width), 1)
    position = jnp.zeros((seqs, width), jnp.int32)
    for s in range(seqs):
        position = jnp.where(row == s, lens[s], position)
    half = HD // 2
    frequency = jnp.exp((lane % half).astype(F32) * (-2.0 / HD * math.log(THETA)))
    angles = position.astype(F32) * frequency
    first = lane % HD < half
    cos_vals = jnp.cos(angles)
    sin_vals = jnp.sin(angles)
    sin_vals = jnp.where(first, -sin_vals, sin_vals)

    def rotate(tile):
        swapped = jnp.where(first, pltpu.roll(tile, width - half, 1), pltpu.roll(tile, half, 1))
        return (tile * cos_vals + swapped * sin_vals).astype(BF16).astype(F32)

    column = lax.broadcasted_iota(jnp.int32, (1, width), 1)
    owner = column % rows // heads
    limit = jnp.zeros((1, width), jnp.int32)
    for s in range(seqs):
        limit = jnp.where(owner == s, lens[s], limit)
    mult = jnp.ones((1, width), F32)
    for j in range(heads):
        mult = jnp.where(column == rows + column % rows // heads * heads + j, lam[j], mult)

    knew = rotate(key_raw).astype(BF16)
    for j in range(heads):
        tile = rotate(query_raw[:, j * width : (j + 1) * width]) * HD ** (-0.5)
        qrows[pl.ds(j, seqs, stride=heads), :] = jnp.where(lane < HD, tile, 0.0)
        qrows[pl.ds(rows + j, seqs, stride=heads), :] = jnp.where(lane < HD, 0.0, tile)
    qcols = jnp.transpose(qrows[...])
    query = jnp.concatenate([jnp.where(owner == s, qcols, 0.0).astype(BF16) for s in range(seqs)], axis=0)
    weights[2].wait()
    vnew = jnp.dot(normed, wv[...], preferred_element_type=F32).astype(BF16).astype(F32)
    for j in range(heads):
        mixed[pl.ds(j, seqs, stride=heads), :] = vnew

    new_row = jnp.concatenate([knew[s : s + 1, :] for s in range(seqs)], axis=1)
    new_row = jnp.broadcast_to(new_row, (16, seqs * width))
    new_score = jnp.dot(new_row, query, preferred_element_type=F32)[:1]
    peak = new_score
    for b in range(BLOCKS):
        if b * block % half_span == 0:
            key_copies[b * block // half_span].wait()
        past = jnp.concatenate([keys[s, pl.ds(b * block, block), :] for s in range(seqs)], axis=1)
        score = jnp.dot(past, query, preferred_element_type=F32)
        place = lax.broadcasted_iota(jnp.int32, (block, width), 0) + b * block
        score = jnp.where(place < limit, score, -jnp.inf)
        scores[pl.ds(b * block, block), :] = score
        peak = jnp.maximum(peak, jnp.max(score, axis=0, keepdims=True))
    expo = jnp.exp(scores[...] - peak)
    expo_new = jnp.exp(new_score - peak)
    factor = mult / (jnp.sum(expo, axis=0, keepdims=True) + expo_new)
    scaled = expo * factor
    weight = jnp.transpose(scaled - pltpu.roll(scaled, rows, 1))[:rows].astype(BF16)
    scaled_new = jnp.broadcast_to(expo_new * factor, (width, width))
    weight_new = jnp.transpose(scaled_new - pltpu.roll(scaled_new, rows, 1))[:rows].astype(BF16).astype(F32)
    pair = 8 // heads
    part = lax.broadcasted_iota(jnp.int32, (8, width), 0) // heads
    for g in range(seqs // pair):
        group = jnp.zeros((8, width), F32)
        for i in range(pair):
            s = g * pair + i
            if s % half_seqs == 0:
                value_copies[s // half_seqs].wait()
            own = jnp.dot(weight[g * 8 : g * 8 + 8], values[s], preferred_element_type=F32)
            group = jnp.where(part == i, own, group)
        where = pl.ds(g * 8, 8)
        mixed[where, :] = group + weight_new[g * 8 : g * 8 + 8] * mixed[where, :]
    mix = mixed[...]
    mix_square = jnp.mean(mix * mix, axis=-1, keepdims=True)
    mixed[...] = mix * lax.rsqrt(mix_square + HEAD_EPS) * head_gain[...] * (1.0 - LAMBDA_BASE)
    head_out = jnp.concatenate([mixed[pl.ds(j, seqs, stride=heads), :] for j in range(heads)], axis=1)
    weights[3].wait()
    out[...] = jnp.dot(head_out.astype(BF16), wo[...], preferred_element_type=F32)


def attention(lens, lam, tokens, mixer_gain, wq, wk, wv, head_gain, wo, cache_keys, cache_values):
    seqs, model_width = tokens.shape
    span, width = cache_keys.shape[1:]
    heads = lam.shape[0]
    vmem = pl.BlockSpec(memory_space=pltpu.VMEM)
    hbm = pl.BlockSpec(memory_space=pltpu.HBM)
    operands = (lens, lam, tokens, mixer_gain, wq, wk, wv, head_gain, wo, cache_keys, cache_values)
    operands = [pltpu.with_memory_space_constraint(x, pltpu.HBM) for x in operands]
    return pl.pallas_call(
        attention_body,
        out_shape=pltpu.VMEM((seqs, model_width), F32),
        in_specs=[hbm] * 11,
        out_specs=vmem,
        scratch_shapes=[
            pltpu.SMEM(lens.shape, jnp.int32),
            pltpu.SMEM(lam.shape, F32),
            pltpu.VMEM(tokens.shape, BF16),
            pltpu.VMEM(mixer_gain.shape, F32),
            pltpu.VMEM(head_gain.shape, F32),
            pltpu.VMEM(wq.shape, BF16),
            pltpu.VMEM(wk.shape, BF16),
            pltpu.VMEM(wv.shape, BF16),
            pltpu.VMEM(wo.shape, BF16),
            pltpu.VMEM((seqs, span, width), BF16),
            pltpu.VMEM((seqs, span, width), BF16),
            pltpu.VMEM((2 * seqs * heads, width), F32),
            pltpu.VMEM((span, width), F32),
            pltpu.VMEM((seqs * heads, width), F32),
            pltpu.SemaphoreType.DMA((5,)),
            pltpu.SemaphoreType.DMA((4,)),
            pltpu.SemaphoreType.DMA((2,)),
            pltpu.SemaphoreType.DMA((2,)),
        ],
        compiler_params=pltpu.CompilerParams(vmem_limit_bytes=20 * 1024 * 1024),
        cost_estimate=pl.CostEstimate(flops=10**9, bytes_accessed=12 * 1024 * 1024, transcendentals=10**6),
        name="attention",
    )(*operands)


EP = ("zh", "zl", "yh", "yl", "xh", "xl")
VMEM = pl.BlockSpec(memory_space=pltpu.VMEM)


def call(body, out_shape, in_specs, scratch=(), flops=10**8):
    return pl.pallas_call(
        body,
        out_shape=out_shape,
        in_specs=in_specs,
        out_specs=jax.tree.map(lambda _: VMEM, out_shape),
        scratch_shapes=list(scratch),
        compiler_params=pltpu.CompilerParams(vmem_limit_bytes=12 * 1024 * 1024),
        cost_estimate=pl.CostEstimate(flops=flops, bytes_accessed=2 * 1024 * 1024, transcendentals=10**5),
    )


def mid_body(tokens, own, other, channel_gain, ids, shares, branch_gate, send, mid, pick, gate, slab):
    seqs, model_width = tokens.shape
    peers, lines, width = send.shape
    chunks = model_width // width
    summed = (tokens[...].astype(F32) + (own[...] + other[...])).astype(BF16)
    mid[...] = summed
    wide = summed.astype(F32)
    mean_square = jnp.mean(wide * wide, axis=-1, keepdims=True)
    ffn = (wide * lax.rsqrt(mean_square + NORM_EPS) * channel_gain[...]).astype(BF16)
    logit = jnp.sum(ffn.astype(F32) * branch_gate[...], axis=-1, keepdims=True)
    gate[...] = jnp.broadcast_to(jax.nn.sigmoid(logit), gate.shape)

    peer = lax.broadcasted_iota(jnp.int32, (seqs, peers), 1)
    row = lax.broadcasted_iota(jnp.int32, (seqs, peers), 0)
    share = jnp.zeros((seqs, peers), F32)
    picked = jnp.zeros((seqs, peers), F32)
    names, parts = jnp.transpose(ids[...].astype(F32)), jnp.transpose(shares[...].astype(F32))
    peer_name = peer.astype(F32)
    for k in range(ids.shape[0]):
        named = names[:, k : k + 1] == peer_name
        picked = jnp.where(named, 1.0, picked)
        share = jnp.where(named, parts[:, k : k + 1], share)
    above = lax.broadcasted_iota(jnp.int32, (seqs, seqs), 0) >= lax.broadcasted_iota(jnp.int32, (seqs, seqs), 1)
    rank = jnp.dot(above.astype(BF16), picked.astype(BF16), preferred_element_type=F32)
    placed = (picked > 0.0) & (rank == (lax.axis_index("tp") + 1).astype(F32))
    pick[...] = jnp.where(placed, share, 0.0).astype(BF16)
    dense = row == 2 * member(peer) + lax.axis_index("tp")
    for r, chosen in enumerate((placed, dense)):
        lines_out = lax.dot_general(
            chosen.astype(F32).astype(BF16), ffn, (((0,), (0,)), ((), ())), preferred_element_type=F32
        )
        for k in range(chunks):
            slab[pl.ds(r * chunks + k, peers, stride=lines), :] = lines_out[:, k * width : (k + 1) * width]
    send[...] = slab[...].reshape(send.shape).astype(BF16)


def member(peer):
    return (peer // 16 % 2) * 4 + (peer // 4 % 2) * 2 + peer % 2


def unpack(slab, first, chunks, lines):
    peers = slab.shape[0] // lines
    return [slab[pl.ds(first + k, peers, stride=lines), :].astype(BF16) for k in range(chunks)]


def experts_body(
    arrived, gate_own, gate_other, up_own, up_other, dense_own, dense_other, down_own, down_other, out, slab,
    down_late, sem,
):
    late = pltpu.make_async_copy(down_other, down_late, sem)
    late.start()
    peers, lines, width = arrived.shape
    chunks = lines // 2
    slab[...] = arrived[...].reshape(slab.shape).astype(F32)
    routed = jnp.concatenate(unpack(slab, 0, chunks, lines), axis=1)
    tokens = unpack(slab, chunks, chunks, lines)
    low, high = jnp.concatenate(tokens[: chunks // 2], axis=1), jnp.concatenate(tokens[chunks // 2 :], axis=1)
    is_first = lax.axis_index("tp") == 0
    blocks, stacked, half_width = dense_own.shape
    units = stacked // 3

    def part(ref, i):
        return ref[:, i * units : (i + 1) * units, :].reshape(blocks * units, half_width)

    mine, theirs = jnp.where(is_first, low, high), jnp.where(is_first, high, low)

    def project(i):
        dims = (((1,), (1,)), ((), ()))
        return lax.dot_general(mine, part(dense_own, i), dims, preferred_element_type=F32) + lax.dot_general(
            theirs, part(dense_other, i), dims, preferred_element_type=F32
        )

    hidden = (jax.nn.silu(project(0)) * project(1)).astype(BF16)
    sum_own = jnp.dot(hidden, part(dense_own, 2), preferred_element_type=F32)
    sum_other = jnp.dot(hidden, part(dense_other, 2), preferred_element_type=F32)
    halves = (jnp.where(is_first, sum_own, sum_other), jnp.where(is_first, sum_other, sum_own))
    for h, value in enumerate(halves):
        for k in range(chunks // 2):
            where = pl.ds(chunks + h * chunks // 2 + k, peers, stride=lines)
            slab[where, :] = value[:, k * width : (k + 1) * width]
    result = jnp.zeros((peers, chunks * width), F32)
    for w_gate, w_up, w_down in ((gate_own, up_own, down_own), (gate_other, up_other, down_late)):
        gate_part = jnp.dot(routed, w_gate[0], preferred_element_type=F32)
        up_part = jnp.dot(routed, w_up[0], preferred_element_type=F32)
        hidden = (jax.nn.silu(gate_part) * up_part).astype(BF16)
        if w_down is down_late:
            late.wait()
        result = result + jnp.dot(hidden, w_down[0], preferred_element_type=F32)
    for k in range(chunks):
        slab[pl.ds(k, peers, stride=lines), :] = result[:, k * width : (k + 1) * width]
    out[...] = slab[...].reshape(out.shape).astype(BF16)


def combine_body(returned, pick, gate, mid, keep, send, slab):
    peers, lines, width = returned.shape
    chunks = lines // 2
    seqs = pick.shape[0]
    slab[...] = returned[...].reshape(slab.shape).astype(F32)
    peer = lax.broadcasted_iota(jnp.int32, (seqs, peers), 1)
    row = lax.broadcasted_iota(jnp.int32, (seqs, peers), 0)
    dense = (row == 2 * member(peer) + lax.axis_index("tp")).astype(F32).astype(BF16)
    routed = jnp.dot(pick[...], jnp.concatenate(unpack(slab, 0, chunks, lines), axis=1), preferred_element_type=F32)
    branch = jnp.dot(dense, jnp.concatenate(unpack(slab, chunks, chunks, lines), axis=1), preferred_element_type=F32)
    total = routed + gate[:, :1] * branch
    half = chunks * width // 2
    is_first = lax.axis_index("tp") == 0
    low, high = total[:, :half], total[:, half:]
    resid = mid[...].astype(F32)
    keep[...] = jnp.where(is_first, resid[:, :half] + low, resid[:, half:] + high)
    send[...] = jnp.where(is_first, high, low)


def swap(value, axis):
    return lax.ppermute(value, axis, [(0, 1), (1, 0)])


def layer(
    tokens, mixer_gain, query_weight, key_weight, value_weight, head_lambda, head_gain, out_weight,
    cache_keys, cache_values, seq_lengths, channel_gain, expert_ids, expert_shares,
    expert_gate, expert_up, expert_down, dense_gate, dense_up, dense_down, branch_gate,
):
    seqs, model_width = tokens.shape
    peers = lax.axis_size(EP)
    width = 2 * HD
    lines = 2 * model_width // width
    half = model_width // 2
    sds = jax.ShapeDtypeStruct
    slab = pltpu.VMEM((peers * lines, width), F32)

    gate_other, up_other, down_other = (swap(w, "tp") for w in (expert_gate, expert_up, expert_down))

    first = jnp.concatenate([dense_gate.T, dense_up.T, dense_down], axis=0)[None]
    second = swap(first, "zl")
    own = attention(
        seq_lengths, head_lambda, tokens, mixer_gain.reshape(1, -1), query_weight, key_weight, value_weight,
        head_gain.reshape(1, -1), out_weight, cache_keys, cache_values,
    )
    other = swap(own, "tp")
    pair = jnp.concatenate([first, second], axis=0)
    pair_y = swap(pair, "yl")
    pair_x = swap(pair, "xl")
    cut_y, cut_x = pair_y[:1], pair_x[1:]
    corner_x = swap(cut_y, "xl")
    corner_y = swap(cut_x, "yl")
    gathered = jnp.concatenate([pair, pair_y, pair_x, corner_x, corner_y], axis=0)
    gathered_other = swap(gathered, "tp")
    middle = call(
        mid_body,
        (
            sds((peers, lines, width), BF16),
            sds((seqs, model_width), BF16),
            sds((seqs, peers), BF16),
            sds((seqs, width), F32),
        ),
        [VMEM] * 7,
        [slab],
    )
    send, mid, pick, gate = middle(
        tokens, own, other, channel_gain.reshape(1, -1), expert_ids.T, expert_shares.T, branch_gate.reshape(1, -1)
    )
    arrived = lax.all_to_all(send, EP, 0, 0, tiled=True)
    down_other = pltpu.with_memory_space_constraint(down_other, pltpu.HBM)
    rows_out = call(
        experts_body,
        sds((peers, lines, width), BF16),
        [VMEM] * 8 + [pl.BlockSpec(memory_space=pltpu.HBM)],
        [slab, pltpu.VMEM(expert_down.shape, BF16), pltpu.SemaphoreType.DMA(())],
    )(arrived, expert_gate, gate_other, expert_up, up_other, gathered, gathered_other, expert_down, down_other)
    returned = lax.all_to_all(rows_out, EP, 0, 0, tiled=True)
    keep, give = call(
        combine_body, (sds((seqs, half), F32), sds((seqs, half), F32)), [VMEM] * 4, [slab]
    )(returned, pick, gate, mid)
    return (keep + swap(give, "tp")).astype(BF16)


def solution(mesh):
    torus = Mesh(mesh.devices.reshape(4, 2, 2, 2, 2, 2, 2), (*EP, "tp"))
    return jax.shard_map(
        layer,
        mesh=torus,
        in_specs=(
            P(EP, None),
            P(),
            P(None, "tp"),
            P(None, "tp"),
            P(None, "tp"),
            P("tp"),
            P(),
            P("tp", None),
            P(EP, None, "tp"),
            P(EP, None, "tp"),
            P(EP),
            P(),
            P(EP, None),
            P(EP, None),
            P(EP, None, "tp"),
            P(EP, None, "tp"),
            P(EP, "tp", None),
            P("tp", EP),
            P("tp", EP),
            P(EP, "tp"),
            P(),
        ),
        out_specs=P(EP, "tp"),
        check_vma=False,
    )
```
